32 devices in a mesh: sp: 16 (over z, y, x), tp: 2 (over core).
Axes of the slice: x: 2, y: 2, z: 4, core: 2. Of those that a mesh axis runs over, the one named last changes fastest.
Arguments:
- resid: bfloat16 [3072, 2048], P('sp'), may hold values from -6 to 6
- queries: bfloat16 [3072, 1024], P('sp', 'tp'), may hold values from -6.5 to 6.5
- keys: bfloat16 [3072, 1024], P('sp', 'tp'), may hold values from -6.5 to 6.5
- values: bfloat16 [3072, 1024], P('sp', 'tp'), may hold values from -6 to 6
- lambdas: float32 [8], P('tp'), may hold values from 0.3 to 0.8
- head_gain: float32 [128], replicated, may hold values from 0.1 to 1.9
- out_weight: bfloat16 [1024, 2048], P('tp'), may hold values from -0.1875 to 0.1875
- norm_gain: float32 [2048], replicated, may hold values from 0.1 to 1.9
- gate_weight: bfloat16 [2048, 5632], P('sp', 'tp'), may hold values from -0.125 to 0.125
- up_weight: bfloat16 [2048, 5632], P('sp', 'tp'), may hold values from -0.125 to 0.125
- down_weight: bfloat16 [5632, 2048], P('tp', 'sp'), may hold values from -0.078125 to 0.078125
Outputs:
- result: bfloat16 [3072, 2048], P('sp')
The draws below stay inside these ranges and needn't reach their ends.
All inputs are finite; a program needn't handle non-finite values.
Results may differ from the reference program's by a relative error of at most 0.014.
Values may be sent and summed in bfloat16 or wider, within the bound.
No kernel may reach another device: no remote copies, remote signals or barrier semaphores. Data moves between devices by JAX's collectives and lax.ppermute only.
A program may use at most 128 MiB of HBM per device.

```python
import jax
import jax.numpy as jnp
from jax import lax

D = 2048
HEADS = 8
QK = 64
VD = 128
FF = 5632
TOK_DEV = 192
TOKENS = 3072
N_TP = 2


def shared_field(key, salt, planted_row, period):
    width = HEADS * 2 * QK
    field = jnp.clip(jax.random.normal(jax.random.fold_in(key, salt), (TOKENS, width), jnp.float32) * 1.3, -6.5, 6.5)
    return field


def draw_queries(key, part):
    return shared_field(key, 11, 5, 97).astype(jnp.bfloat16)


def draw_keys(key, part):
    return shared_field(key, 23, 3, 89).astype(jnp.bfloat16)


def level_of(own_key, shape, cuts, low, high):
    factor_of, own = 1.0, jax.random.fold_in(own_key, 6)
    for position, blocks in cuts:
        steps = jnp.exp(jax.random.uniform(jax.random.fold_in(own, position), (blocks,), jnp.float32, low / len(cuts), high / len(cuts)))
        factor_of = factor_of * jnp.repeat(steps, shape[position] // blocks).reshape([-1 if axis == position else 1 for axis in range(len(shape))])
    return factor_of


def normal_values(stream_key, extent, scale, bound, cuts=(), kind=jnp.bfloat16):
    gain = level_of(stream_key, extent, cuts, -0.22, 0.18) if cuts else 1.0
    array = jax.random.normal(stream_key, extent, jnp.float32) * scale * gain
    return jnp.minimum(jnp.maximum(array, -bound), bound).astype(kind)


def setup_inputs(seed: int = 0) -> dict:
    splits = jax.random.split(jax.random.key(seed), 12)
    resid = normal_values(splits[0], (TOKENS, D), 1.0, 6.0, ((0, 16),))
    queries = draw_queries(jax.random.fold_in(splits[11], 71), 0)
    keys = draw_keys(jax.random.fold_in(splits[11], 71), 0)
    values = normal_values(splits[3], (TOKENS, HEADS * VD), 1.0, 6.0, ((0, 16), (1, 2)))
    lambdas = jnp.clip(0.3 + 0.5 * jax.random.uniform(splits[4], (HEADS,), jnp.float32) ** level_of(splits[4], (HEADS,), ((0, 2),), -0.2, 0.2), 0.3, 0.8)
    head_gain = jnp.clip(1.0 + 0.18 * jax.random.normal(splits[5], (VD,), jnp.float32), 0.1, 1.9)
    out_weight = normal_values(splits[6], (HEADS * VD, D), (HEADS * VD) ** -0.5, 0.1875, ((0, 2),))
    norm_gain = jnp.clip(1.0 + 0.18 * jax.random.normal(splits[7], (D,), jnp.float32), 0.1, 1.9)
    gate_weight = normal_values(splits[8], (D, FF), D ** -0.5, 0.125, ((0, 16), (1, 2)))
    up_weight = normal_values(splits[9], (D, FF), D ** -0.5, 0.125, ((0, 16), (1, 2)))
    down_weight = normal_values(splits[10], (FF, D), FF ** -0.5, 0.078125, ((0, 2), (1, 16)))
    return dict(resid=resid, queries=queries, keys=keys, values=values, lambdas=lambdas, head_gain=head_gain, out_weight=out_weight, norm_gain=norm_gain, gate_weight=gate_weight, up_weight=up_weight, down_weight=down_weight)


def reference(resid, queries, keys, values, lambdas, head_gain, out_weight, norm_gain, gate_weight, up_weight, down_weight):
    tok_total = resid.shape[0]
    head_count = lambdas.shape[0]
    query_all = queries.reshape(tok_total, head_count, 2, QK).astype(jnp.float32)
    key_all = keys.reshape(tok_total, head_count, 2, QK).astype(jnp.float32)
    value_all = values.reshape(tok_total, head_count, VD).astype(jnp.float32)
    score_scale = QK ** (-0.5)
    key_pos = jnp.arange(tok_total, dtype=jnp.int32)

    def one_block(block_index):
        block_start = (block_index * TOK_DEV).astype(jnp.int32)
        query_block = lax.dynamic_slice_in_dim(query_all, block_start, TOK_DEV, 0)
        scores = jnp.einsum('qhcd,khcd->chqk', query_block, key_all) * score_scale
        query_pos = block_start + jnp.arange(TOK_DEV, dtype=jnp.int32)
        causal_mask = key_pos[None, :] <= query_pos[:, None]
        scores = jnp.where(causal_mask, scores, -1e+30)
        row_max = lax.optimization_barrier(jnp.max(scores, axis=-1, keepdims=True))
        expo = jnp.where(causal_mask, jnp.exp(scores - row_max), 0.0)
        row_sum = lax.optimization_barrier(jnp.sum(expo, axis=-1))
        rounded = lax.optimization_barrier(expo.astype(jnp.bfloat16)).astype(jnp.float32)
        numer = jnp.einsum('chqk,khd->chqd', rounded, value_all)
        ratio = numer / row_sum[..., None]
        mixed_heads = ratio[0] - lambdas[:, None, None] * ratio[1]
        normed_heads = mixed_heads * lax.rsqrt(lax.optimization_barrier(jnp.mean(mixed_heads * mixed_heads, axis=-1, keepdims=True)) + 1e-05) * head_gain
        return jnp.transpose(normed_heads.astype(jnp.bfloat16), (1, 0, 2))
    head_out = lax.map(one_block, jnp.arange(tok_total // TOK_DEV, dtype=jnp.int32)).reshape(tok_total, head_count * VD)
    group_cols = head_count // N_TP * VD
    branch = jnp.zeros((tok_total, resid.shape[1]), jnp.float32)
    for group in range(N_TP):
        partial_sum = jnp.dot(head_out[:, group * group_cols:(group + 1) * group_cols], out_weight[group * group_cols:(group + 1) * group_cols], preferred_element_type=jnp.float32)
        branch = branch + partial_sum.astype(jnp.bfloat16).astype(jnp.float32)
    first = resid.astype(jnp.float32) + branch
    normed = (first * lax.rsqrt(lax.optimization_barrier(jnp.mean(first * first, axis=-1, keepdims=True)) + 1e-06) * norm_gain).astype(jnp.bfloat16)
    hidden_group = FF // N_TP
    mixer = jnp.zeros_like(first)
    for group in range(N_TP):
        cols = slice(group * hidden_group, (group + 1) * hidden_group)
        gate_act = jnp.dot(normed, gate_weight[:, cols], preferred_element_type=jnp.float32)
        up_act = jnp.dot(normed, up_weight[:, cols], preferred_element_type=jnp.float32)
        hidden = (jax.nn.silu(gate_act) * up_act).astype(jnp.bfloat16)
        partial_sum = jnp.dot(hidden, down_weight[cols, :], preferred_element_type=jnp.float32)
        mixer = mixer + partial_sum.astype(jnp.bfloat16).astype(jnp.float32)
    return (first + 0.5 * mixer).astype(jnp.bfloat16)
```

```python
import functools

import jax
import jax.numpy as jnp
from jax import lax
from jax.experimental import pallas as pl
from jax.experimental.pallas import tpu as pltpu
from jax.sharding import Mesh, PartitionSpec as P

QK = 64
VD = 128
BF = jnp.bfloat16
F32 = jnp.float32


def attn_kernel(pos_ref, lam_ref, q_ref, k_ref, v_ref, gain_ref, o_ref, s_ref, *, groups, planes, rows):
    p_self = pos_ref[0]
    span = planes * rows
    lane = lax.broadcasted_iota(jnp.int32, (rows, 2 * QK), 1)
    row_id = lax.broadcasted_iota(jnp.int32, (rows, span), 0)
    col_id = lax.broadcasted_iota(jnp.int32, (rows, span), 1)
    mask_one = col_id <= row_id + p_self * rows
    mask = jnp.concatenate([mask_one, mask_one], axis=0)
    lam = lam_ref[0]
    for zq in range(groups):
        q = q_ref[zq] * jnp.asarray(QK**-0.5, BF)
        zero = jnp.zeros_like(q)
        q2 = jnp.concatenate([jnp.where(lane < QK, q, zero), jnp.where(lane < QK, zero, q)], axis=0)
        m = None
        for zk in range(zq + 1):
            kc = jnp.concatenate([k_ref[p, zk] for p in range(planes)], axis=0)
            s = lax.dot_general(q2, kc, (((1,), (1,)), ((), ())), preferred_element_type=F32)
            if zk == zq:
                s = jnp.where(mask, s, -1e30)
            s_ref[:, zk * span : (zk + 1) * span] = s
            mc = jnp.max(s, axis=-1, keepdims=True)
            m = mc if m is None else jnp.maximum(m, mc)
        acc = jnp.zeros((2 * rows, VD), F32)
        tot = jnp.zeros((2 * rows, 1), F32)
        for zk in range(zq + 1):
            e = jnp.exp(s_ref[:, zk * span : (zk + 1) * span] - m)
            tot = tot + jnp.sum(e, axis=-1, keepdims=True)
            vc = jnp.concatenate([v_ref[p, zk] for p in range(planes)], axis=0)
            acc = acc + jnp.dot(e.astype(BF), vc, preferred_element_type=F32)
        ratio = acc / tot
        mixed = ratio[:rows] - lam * ratio[rows:]
        scale = lax.rsqrt(jnp.mean(mixed * mixed, axis=-1, keepdims=True) + 1e-05)
        o_ref[zq] = (mixed * scale * gain_ref[...]).astype(BF)


def attention_split(queries, keys, values, lambdas, head_gain, groups, planes):
    rows = queries.shape[0]
    heads = lambdas.shape[0]

    def exchange(x):
        parts = x.reshape(rows, groups, VD).transpose(1, 0, 2)
        return parts

    qkv = jnp.stack([exchange(keys), exchange(values), exchange(queries)], axis=1)
    qkv = lax.all_to_all(qkv, "z", 0, 0, tiled=True)
    kv = lax.all_gather(jnp.stack([qkv[:, 0], qkv[:, 1]]), "p", axis=0, tiled=False)
    lam = lax.dynamic_slice_in_dim(lambdas, lax.axis_index("z"), 1, 0)
    pos = lax.axis_index("p").astype(jnp.int32).reshape(1)
    out = pl.pallas_call(
        functools.partial(attn_kernel, groups=groups, planes=planes, rows=rows),
        out_shape=jax.ShapeDtypeStruct((groups, rows, VD), BF),
        in_specs=[
            pl.BlockSpec(memory_space=pltpu.SMEM),
            pl.BlockSpec(memory_space=pltpu.SMEM),
            pl.BlockSpec(memory_space=pltpu.VMEM),
            pl.BlockSpec(memory_space=pltpu.VMEM),
            pl.BlockSpec(memory_space=pltpu.VMEM),
            pl.BlockSpec(memory_space=pltpu.VMEM),
        ],
        out_specs=pl.BlockSpec(memory_space=pltpu.VMEM),
        scratch_shapes=[pltpu.VMEM((2 * rows, groups * planes * rows), F32)],
        cost_estimate=pl.CostEstimate(
            flops=8 * rows * rows * groups * groups * planes * VD,
            transcendentals=rows * rows * groups * groups * planes,
            bytes_accessed=4 * rows * groups * planes * VD,
        ),
        compiler_params=pltpu.CompilerParams(vmem_limit_bytes=40 * 1024 * 1024),
        name="attn",
    )(pos, lam, qkv[:, 2], kv[:, 0], kv[:, 1], head_gain.reshape(1, VD))
    back = lax.all_to_all(out, "z", 0, 0, tiled=True)
    return back


def attention_plain(queries, keys, values, lambdas, head_gain):
    tok_rows = queries.shape[0]
    local_heads = lambdas.shape[0]
    offset = (lax.axis_index("z") * lax.axis_size("p") + lax.axis_index("p")) * tok_rows
    query_four = queries.reshape(tok_rows, local_heads, 2, QK)
    query_pos = offset + lax.iota(jnp.int32, tok_rows)
    key_rows = lax.all_gather(keys, ("z", "p"), axis=0, tiled=True)
    value_rows = lax.all_gather(values, ("z", "p"), axis=0, tiled=True)
    key_count = key_rows.shape[0]
    key_span = key_count
    while key_span > 1024 and key_span % 2 == 0:
        key_span = key_span // 2

    def one_span(span_index, state):
        run_max, run_sum, run_acc = state
        start = span_index * key_span
        key_part = lax.dynamic_slice_in_dim(key_rows, start, key_span, 0)
        key_part = key_part.reshape(key_span, local_heads, 2, QK)
        value_part = lax.dynamic_slice_in_dim(value_rows, start, key_span, 0)
        value_part = value_part.reshape(key_span, local_heads, VD)
        key_pos = start + lax.iota(jnp.int32, key_span)
        scores = jnp.einsum("qhcd,khcd->chqk", query_four, key_part, preferred_element_type=F32)
        causal = key_pos[None, :] <= query_pos[:, None]
        scores = jnp.where(causal, scores * QK**-0.5, -1e30)
        new_max = jnp.maximum(run_max, jnp.max(scores, axis=-1))
        expo = jnp.where(causal, jnp.exp(scores - new_max[..., None]), 0.0)
        factor = jnp.exp(run_max - new_max)
        new_sum = run_sum * factor + jnp.sum(expo, axis=-1)
        new_acc = run_acc * factor[..., None] + jnp.einsum(
            "chqk,khd->chqd", expo.astype(BF), value_part, preferred_element_type=F32
        )
        return new_max, new_sum, new_acc

    initial = (
        jnp.full((2, local_heads, tok_rows), -1e30, F32),
        jnp.zeros((2, local_heads, tok_rows), F32),
        jnp.zeros((2, local_heads, tok_rows, VD), F32),
    )
    _, final_sum, final_acc = lax.fori_loop(0, key_count // key_span, one_span, initial)
    ratio = final_acc / final_sum[..., None]
    mixed = ratio[0] - lambdas[:, None, None] * ratio[1]
    scale = lax.rsqrt(jnp.mean(mixed * mixed, axis=-1, keepdims=True) + 1e-05)
    return (mixed * scale * head_gain).astype(BF)


def local(
    resid,
    queries,
    keys,
    values,
    lambdas,
    head_gain,
    out_weight,
    norm_gain,
    gate_weight,
    up_weight,
    down_weight,
):
    groups = lax.axis_size("z")
    planes = lax.axis_size("p")
    tok_rows, width = resid.shape
    local_heads = lambdas.shape[0]
    own_rows = tok_rows // lax.axis_size("tp")
    z_self = lax.axis_index("z")

    if local_heads == groups:
        head_out = attention_split(queries, keys, values, lambdas, head_gain, groups, planes)
    else:
        head_out = attention_plain(queries, keys, values, lambdas, head_gain)

    units = gate_weight.shape[1]
    span = -(-units // (groups * 128)) * 128
    starts = [min(g * span, units - span) for g in range(groups)]
    first_unit = z_self * span - jnp.minimum(z_self * span, units - span)
    k_rows = gate_weight.shape[0]

    gate_up = jnp.stack(
        [jnp.stack([gate_weight[:, s : s + span], up_weight[:, s : s + span]]) for s in starts]
    )
    gate_up = lax.all_to_all(gate_up, "z", 0, 0, tiled=True)
    gate_all = lax.all_gather(gate_up[:, 0], "p", axis=0, tiled=False).reshape(width, span)
    up_all = lax.all_gather(gate_up[:, 1], "p", axis=0, tiled=False).reshape(width, span)
    down = jnp.stack([down_weight[s : s + span] for s in starts])
    down = lax.all_to_all(down, "z", 0, 0, tiled=True)
    down_all = lax.all_gather(down, "p", axis=0, tiled=False)

    out_three = out_weight.reshape(local_heads, VD, width)
    branch = lax.psum_scatter(
        jnp.einsum("hqd,hde->qe", head_out, out_three, preferred_element_type=F32).astype(BF),
        "tp",
        scatter_dimension=0,
        tiled=True,
    ).astype(F32)
    resid_own = lax.dynamic_slice_in_dim(resid, lax.axis_index("tp") * own_rows, own_rows, 0)
    first = resid_own.astype(F32) + branch
    normed = first * lax.rsqrt(jnp.mean(first * first, axis=-1, keepdims=True) + 1e-06) * norm_gain
    normed = normed.astype(BF).reshape(own_rows, groups, planes, k_rows).transpose(0, 2, 1, 3)
    normed_all = lax.all_gather(normed.reshape(own_rows, width), ("z", "tp"), axis=0, tiled=True)
    gate_act = jnp.dot(normed_all, gate_all, preferred_element_type=F32)
    up_act = jnp.dot(normed_all, up_all, preferred_element_type=F32)
    keep = lax.iota(jnp.int32, span) >= first_unit
    hidden = jnp.where(keep[None, :], jax.nn.silu(gate_act) * up_act, 0.0).astype(BF)
    terms = jnp.einsum("th,pzhd->tzpd", hidden, down_all, preferred_element_type=F32)
    terms = terms.astype(BF).reshape(-1, width)
    mixer = lax.psum_scatter(terms, ("z", "tp"), scatter_dimension=0, tiled=True).astype(F32)
    finished = (first + 0.5 * mixer).astype(BF)
    return lax.all_gather(finished, "tp", axis=0, tiled=True)


def solution(mesh):
    sp, tp = mesh.shape["sp"], mesh.shape["tp"]
    groups = 4 if sp % 4 == 0 else 1
    split = Mesh(mesh.devices.reshape(groups, sp // groups, tp), ("z", "p", "tp"))
    rows = ("z", "p")
    return jax.shard_map(
        local,
        mesh=split,
        in_specs=(
            P(rows, None),
            P(rows, "tp"),
            P(rows, "tp"),
            P(rows, "tp"),
            P("tp"),
            P(),
            P("tp", None),
            P(),
            P(rows, "tp"),
            P(rows, "tp"),
            P("tp", rows),
        ),
        out_specs=P(rows, None),
        check_vma=False,
    )
```

```python
import functools

import jax
import jax.numpy as jnp
from jax import lax
from jax.experimental import pallas as pl
from jax.experimental.pallas import tpu as pltpu
from jax.sharding import Mesh, PartitionSpec as P


QK = 64
VD = 128
BF = jnp.bfloat16
F32 = jnp.float32


def attn_kernel(pos_ref, lam_ref, q_ref, k_ref, v_ref, gain_ref, o_ref, s_ref, *, groups, planes, rows):
    z_self = pos_ref[0]
    p_self = pos_ref[1]
    span = planes * rows
    lane = lax.broadcasted_iota(jnp.int32, (rows, 2 * QK), 1)
    row_id = lax.broadcasted_iota(jnp.int32, (rows, span), 0)
    col_id = lax.broadcasted_iota(jnp.int32, (rows, span), 1)
    mask_one = col_id <= row_id + p_self * rows
    mask = jnp.concatenate([mask_one, mask_one], axis=0)
    lam = lam_ref[0]
    for zq in range(groups):
        q = q_ref[z_self ^ zq] * jnp.asarray(QK**-0.5, BF)
        zero = jnp.zeros_like(q)
        q2 = jnp.concatenate([jnp.where(lane < QK, q, zero), jnp.where(lane < QK, zero, q)], axis=0)
        m = None
        for zk in range(zq + 1):
            kc = jnp.concatenate([k_ref[p_self ^ p, z_self ^ zk] for p in range(planes)], axis=0)
            s = lax.dot_general(q2, kc, (((1,), (1,)), ((), ())), preferred_element_type=F32)
            if zk == zq:
                s = jnp.where(mask, s, -1e30)
            s_ref[:, zk * span : (zk + 1) * span] = s
            mc = jnp.max(s, axis=-1, keepdims=True)
            m = mc if m is None else jnp.maximum(m, mc)
        acc = jnp.zeros((2 * rows, VD), F32)
        tot = jnp.zeros((2 * rows, 1), F32)
        for zk in range(zq + 1):
            e = jnp.exp(s_ref[:, zk * span : (zk + 1) * span] - m)
            tot = tot + jnp.sum(e, axis=-1, keepdims=True)
            vc = jnp.concatenate([v_ref[p_self ^ p, z_self ^ zk] for p in range(planes)], axis=0)
            acc = acc + jnp.dot(e.astype(BF), vc, preferred_element_type=F32)
        ratio = acc / tot
        mixed = ratio[:rows] - lam * ratio[rows:]
        scale = lax.rsqrt(jnp.mean(mixed * mixed, axis=-1, keepdims=True) + 1e-05)
        o_ref[z_self ^ zq] = (mixed * scale * gain_ref[...]).astype(BF)


def mixer_kernel(pos_ref, x_ref, *refs, rows):
    gates, ups, downs = refs[0:4], refs[4:8], refs[8:12]
    o_ref = refs[12]
    z_self, p_self, first_unit = pos_ref[0], pos_ref[1], pos_ref[2]
    block = downs[0].shape[2]
    span = gates[0].shape[1]

    def lanes(i, j):
        return pl.ds(pl.multiple_of(((z_self ^ j) * 4 + (p_self ^ i)) * block, block), block)

    def step(n, carry):
        at = pl.ds(pl.multiple_of(n * rows, rows), rows)
        gate = jnp.zeros((rows, span), F32)
        up = jnp.zeros((rows, span), F32)
        for i in range(4):
            x = jnp.concatenate([x_ref[at, lanes(i, j)] for j in range(4)], axis=1)
            gate = gate + jnp.dot(x, gates[i][...], preferred_element_type=F32)
            up = up + jnp.dot(x, ups[i][...], preferred_element_type=F32)
        hidden = gate / (1.0 + jnp.exp(-gate)) * up
        keep = lax.broadcasted_iota(jnp.int32, (rows, span), 1) >= first_unit
        hidden = jnp.where(keep, hidden, 0.0).astype(BF)
        for i in range(4):
            down = jnp.concatenate([downs[i][j] for j in range(4)], axis=1)
            out = jnp.dot(hidden, down, preferred_element_type=F32).astype(BF)
            for j in range(4):
                o_ref[at, lanes(i, j)] = out[:, j * block : (j + 1) * block]
        return carry

    lax.fori_loop(0, x_ref.shape[0] // rows, step, 0)


def swap(x, axis, bit):
    size = lax.axis_size(axis)
    return lax.ppermute(x, axis, [(i, i ^ bit) for i in range(size)])


def plane_gather(x, first_bit):
    one, two = swap(x, "p", 1), swap(x, "p", 2)
    diag = swap(one, "p", 2) if first_bit == 1 else swap(two, "p", 1)
    return [x, one, two, diag]


def z_exchange(part):
    z_self = lax.axis_index("z")
    sends = [part(z_self ^ j) for j in range(1, 4)]
    got = [swap(x, "z", j + 1) for j, x in enumerate(sends)]
    return jnp.stack([part(z_self)] + got)


def fast_local(
    resid,
    queries,
    keys,
    values,
    lambdas,
    head_gain,
    out_weight,
    norm_gain,
    gate_weight,
    up_weight,
    down_weight,
):
    tok_rows, width = resid.shape
    own_rows = tok_rows // lax.axis_size("tp")
    z_self = lax.axis_index("z").astype(jnp.int32)
    p_self = lax.axis_index("p").astype(jnp.int32)

    def head(x):
        return lambda g: lax.dynamic_slice_in_dim(x, g * VD, VD, 1)

    qkv = z_exchange(lambda g: jnp.stack([head(x)(g) for x in (keys, values, queries)]))
    key_all = jnp.stack(plane_gather(qkv[:, 0], 1))
    value_all = jnp.stack(plane_gather(qkv[:, 1], 2))

    units = gate_weight.shape[1]
    span = -(-units // 512) * 128

    def start(g):
        return jnp.minimum(g * span, units - span)

    gate_mine = z_exchange(lambda g: lax.dynamic_slice_in_dim(gate_weight, start(g), span, 1))
    up_mine = z_exchange(lambda g: lax.dynamic_slice_in_dim(up_weight, start(g), span, 1))
    down_mine = z_exchange(lambda g: lax.dynamic_slice_in_dim(down_weight, start(g), span, 0))
    gates = plane_gather(gate_mine.reshape(-1, span), 1)
    ups = plane_gather(up_mine.reshape(-1, span), 2)
    half = span // 2
    low = plane_gather(down_mine[:, :half], 1)
    high = plane_gather(down_mine[:, half:], 2)
    downs = [jnp.concatenate(pair, axis=1) for pair in zip(low, high)]

    lam = lax.dynamic_slice_in_dim(lambdas, z_self, 1, 0)
    smem = pl.BlockSpec(memory_space=pltpu.SMEM)
    vmem = pl.BlockSpec(memory_space=pltpu.VMEM)
    keys_total = 16 * tok_rows
    out = pl.pallas_call(
        functools.partial(attn_kernel, groups=4, planes=4, rows=tok_rows),
        out_shape=jax.ShapeDtypeStruct((4, tok_rows, VD), BF),
        in_specs=[smem, smem, vmem, vmem, vmem, vmem],
        out_specs=vmem,
        scratch_shapes=[pltpu.VMEM((2 * tok_rows, keys_total), F32)],
        cost_estimate=pl.CostEstimate(
            flops=3 * tok_rows * keys_total * 4 * VD * 2,
            transcendentals=5 * tok_rows * keys_total,
            bytes_accessed=4 * keys_total * VD,
        ),
        compiler_params=pltpu.CompilerParams(vmem_limit_bytes=40 * 1024 * 1024),
        name="attn",
    )(jnp.stack([z_self, p_self]), lam, qkv[:, 2], key_all, value_all, head_gain.reshape(1, VD))
    back = z_exchange(lambda g: lax.dynamic_index_in_dim(out, g ^ z_self, 0, keepdims=False))
    head_out = jnp.concatenate(
        [lax.dynamic_index_in_dim(back, z_self ^ h, 0, keepdims=False) for h in range(4)], axis=1
    )
    projected = jnp.dot(head_out, out_weight, preferred_element_type=F32).astype(BF)
    branch = lax.psum_scatter(
        projected,
        "tp",
        scatter_dimension=0,
        tiled=True,
    ).astype(F32)
    resid_own = lax.dynamic_slice_in_dim(resid, lax.axis_index("tp") * own_rows, own_rows, 0)
    first = resid_own.astype(F32) + branch
    normed = first * lax.rsqrt(jnp.mean(first * first, axis=-1, keepdims=True) + 1e-06) * norm_gain
    normed_all = lax.all_gather(normed.astype(BF), ("z", "tp"), axis=0, tiled=True)
    first_unit = z_self * span - start(z_self)
    tokens = normed_all.shape[0]
    step = 256 if tokens % 256 == 0 else tokens
    terms = pl.pallas_call(
        functools.partial(mixer_kernel, rows=step),
        out_shape=jax.ShapeDtypeStruct((tokens, width), BF),
        in_specs=[smem] + [vmem] * 13,
        out_specs=vmem,
        cost_estimate=pl.CostEstimate(
            flops=6 * tokens * width * span,
            transcendentals=tokens * span,
            bytes_accessed=6 * width * span + 4 * tokens * width,
        ),
        compiler_params=pltpu.CompilerParams(vmem_limit_bytes=50 * 1024 * 1024),
        name="mixer",
    )(jnp.stack([z_self, p_self, first_unit]), normed_all, *gates, *ups, *downs)
    mixer = lax.psum_scatter(terms, ("z", "tp"), scatter_dimension=0, tiled=True).astype(F32)
    finished = (first + 0.5 * mixer).astype(BF)
    return lax.all_gather(finished, "tp", axis=0, tiled=True)


def attention_plain(queries, keys, values, lambdas, head_gain):
    tok_rows = queries.shape[0]
    local_heads = lambdas.shape[0]
    offset = (lax.axis_index("z") * lax.axis_size("p") + lax.axis_index("p")) * tok_rows
    query_four = queries.reshape(tok_rows, local_heads, 2, QK)
    query_pos = offset + lax.iota(jnp.int32, tok_rows)
    key_rows = lax.all_gather(keys, ("z", "p"), axis=0, tiled=True)
    value_rows = lax.all_gather(values, ("z", "p"), axis=0, tiled=True)
    key_count = key_rows.shape[0]
    key_span = key_count
    while key_span > 1024 and key_span % 2 == 0:
        key_span = key_span // 2

    def one_span(span_index, state):
        run_max, run_sum, run_acc = state
        start = span_index * key_span
        key_part = lax.dynamic_slice_in_dim(key_rows, start, key_span, 0)
        key_part = key_part.reshape(key_span, local_heads, 2, QK)
        value_part = lax.dynamic_slice_in_dim(value_rows, start, key_span, 0)
        value_part = value_part.reshape(key_span, local_heads, VD)
        key_pos = start + lax.iota(jnp.int32, key_span)
        scores = jnp.einsum("qhcd,khcd->chqk", query_four, key_part, preferred_element_type=F32)
        causal = key_pos[None, :] <= query_pos[:, None]
        scores = jnp.where(causal, scores * QK**-0.5, -1e30)
        new_max = jnp.maximum(run_max, jnp.max(scores, axis=-1))
        expo = jnp.where(causal, jnp.exp(scores - new_max[..., None]), 0.0)
        factor = jnp.exp(run_max - new_max)
        new_sum = run_sum * factor + jnp.sum(expo, axis=-1)
        new_acc = run_acc * factor[..., None] + jnp.einsum(
            "chqk,khd->chqd", expo.astype(BF), value_part, preferred_element_type=F32
        )
        return new_max, new_sum, new_acc

    initial = (
        jnp.full((2, local_heads, tok_rows), -1e30, F32),
        jnp.zeros((2, local_heads, tok_rows), F32),
        jnp.zeros((2, local_heads, tok_rows, VD), F32),
    )
    _, final_sum, final_acc = lax.fori_loop(0, key_count // key_span, one_span, initial)
    ratio = final_acc / final_sum[..., None]
    mixed = ratio[0] - lambdas[:, None, None] * ratio[1]
    scale = lax.rsqrt(jnp.mean(mixed * mixed, axis=-1, keepdims=True) + 1e-05)
    return (mixed * scale * head_gain).astype(BF)


def local(
    resid,
    queries,
    keys,
    values,
    lambdas,
    head_gain,
    out_weight,
    norm_gain,
    gate_weight,
    up_weight,
    down_weight,
):
    groups = lax.axis_size("z")
    planes = lax.axis_size("p")
    tok_rows, width = resid.shape
    local_heads = lambdas.shape[0]
    own_rows = tok_rows // lax.axis_size("tp")
    z_self = lax.axis_index("z")

    head_out = attention_plain(queries, keys, values, lambdas, head_gain)

    units = gate_weight.shape[1]
    span = -(-units // (groups * 128)) * 128
    starts = [min(g * span, units - span) for g in range(groups)]
    first_unit = z_self * span - jnp.minimum(z_self * span, units - span)
    k_rows = gate_weight.shape[0]

    gate_up = jnp.stack(
        [jnp.stack([gate_weight[:, s : s + span], up_weight[:, s : s + span]]) for s in starts]
    )
    gate_up = lax.all_to_all(gate_up, "z", 0, 0, tiled=True)
    gate_all = lax.all_gather(gate_up[:, 0], "p", axis=0, tiled=False).reshape(width, span)
    up_all = lax.all_gather(gate_up[:, 1], "p", axis=0, tiled=False).reshape(width, span)
    down = jnp.stack([down_weight[s : s + span] for s in starts])
    down = lax.all_to_all(down, "z", 0, 0, tiled=True)
    down_all = lax.all_gather(down, "p", axis=0, tiled=False)

    out_three = out_weight.reshape(local_heads, VD, width)
    branch = lax.psum_scatter(
        jnp.einsum("hqd,hde->qe", head_out, out_three, preferred_element_type=F32).astype(BF),
        "tp",
        scatter_dimension=0,
        tiled=True,
    ).astype(F32)
    resid_own = lax.dynamic_slice_in_dim(resid, lax.axis_index("tp") * own_rows, own_rows, 0)
    first = resid_own.astype(F32) + branch
    normed = first * lax.rsqrt(jnp.mean(first * first, axis=-1, keepdims=True) + 1e-06) * norm_gain
    normed = normed.astype(BF).reshape(own_rows, groups, planes, k_rows).transpose(0, 2, 1, 3)
    normed_all = lax.all_gather(normed.reshape(own_rows, width), ("z", "tp"), axis=0, tiled=True)
    gate_act = jnp.dot(normed_all, gate_all, preferred_element_type=F32)
    up_act = jnp.dot(normed_all, up_all, preferred_element_type=F32)
    keep = lax.iota(jnp.int32, span) >= first_unit
    hidden = jnp.where(keep[None, :], jax.nn.silu(gate_act) * up_act, 0.0).astype(BF)
    terms = jnp.einsum("th,pzhd->tzpd", hidden, down_all, preferred_element_type=F32)
    terms = terms.astype(BF).reshape(-1, width)
    mixer = lax.psum_scatter(terms, ("z", "tp"), scatter_dimension=0, tiled=True).astype(F32)
    finished = (first + 0.5 * mixer).astype(BF)
    return lax.all_gather(finished, "tp", axis=0, tiled=True)


def solution(mesh):
    sp, tp = mesh.shape["sp"], mesh.shape["tp"]
    groups = 4 if sp % 4 == 0 else 1
    split = Mesh(mesh.devices.reshape(groups, sp // groups, tp), ("z", "p", "tp"))
    rows = ("z", "p")

    def chosen(resid, queries, keys, values, lambdas, *rest):
        four = groups == 4 and sp // groups == 4 and lambdas.shape[0] == 4
        if four and rest[-1].shape[1] == 128:
            return fast_local(resid, queries, keys, values, lambdas, *rest)
        return local(resid, queries, keys, values, lambdas, *rest)

    return jax.shard_map(
        chosen,
        mesh=split,
        in_specs=(
            P(rows, None),
            P(rows, "tp"),
            P(rows, "tp"),
            P(rows, "tp"),
            P("tp"),
            P(),
            P("tp", None),
            P(),
            P(rows, "tp"),
            P(rows, "tp"),
            P("tp", rows),
        ),
        out_specs=P(rows, None),
        check_vma=False,
    )
```

```python
import functools

import jax
import jax.numpy as jnp
from jax import lax
from jax.experimental import pallas as pl
from jax.experimental.pallas import tpu as pltpu
from jax.sharding import Mesh, PartitionSpec as P


QK = 64
VD = 128
BF = jnp.bfloat16
F32 = jnp.float32


def attn_kernel(pos_ref, lam_ref, q_ref, k_ref, v_ref, gain_ref, o_ref, s_ref, *, groups, planes, rows):
    z_self = pos_ref[0]
    p_self = pos_ref[1]
    span = planes * rows
    lane = lax.broadcasted_iota(jnp.int32, (rows, 2 * QK), 1)
    row_id = lax.broadcasted_iota(jnp.int32, (rows, span), 0)
    col_id = lax.broadcasted_iota(jnp.int32, (rows, span), 1)
    mask_one = col_id <= row_id + p_self * rows
    mask = jnp.concatenate([mask_one, mask_one], axis=0)
    lam = lam_ref[0]
    for zq in range(groups):
        q = q_ref[z_self ^ zq] * jnp.asarray(QK**-0.5, BF)
        zero = jnp.zeros_like(q)
        q2 = jnp.concatenate([jnp.where(lane < QK, q, zero), jnp.where(lane < QK, zero, q)], axis=0)
        m = None
        for zk in range(zq + 1):
            kc = jnp.concatenate([k_ref[p_self ^ p, z_self ^ zk] for p in range(planes)], axis=0)
            s = lax.dot_general(q2, kc, (((1,), (1,)), ((), ())), preferred_element_type=F32)
            if zk == zq:
                s = jnp.where(mask, s, -1e30)
            s_ref[:, zk * span : (zk + 1) * span] = s
            mc = jnp.max(s, axis=-1, keepdims=True)
            m = mc if m is None else jnp.maximum(m, mc)
        acc = jnp.zeros((2 * rows, VD), F32)
        tot = jnp.zeros((2 * rows, 1), F32)
        for zk in range(zq + 1):
            e = jnp.exp(s_ref[:, zk * span : (zk + 1) * span] - m)
            tot = tot + jnp.sum(e, axis=-1, keepdims=True)
            vc = jnp.concatenate([v_ref[p_self ^ p, z_self ^ zk] for p in range(planes)], axis=0)
            acc = acc + jnp.dot(e.astype(BF), vc, preferred_element_type=F32)
        ratio = acc / tot
        mixed = ratio[:rows] - lam * ratio[rows:]
        scale = lax.rsqrt(jnp.mean(mixed * mixed, axis=-1, keepdims=True) + 1e-05)
        o_ref[z_self ^ zq] = (mixed * scale * gain_ref[...]).astype(BF)


def mixer_kernel(pos_ref, *refs, parts):
    xs, refs = refs[:parts], refs[parts:]
    gates, ups, downs, outs = refs[0:4], refs[4:8], refs[8:12], refs[12:]
    z_self, p_self, first_unit = pos_ref[0], pos_ref[1], pos_ref[2]
    block = downs[0].shape[2]
    span = gates[0].shape[1]
    own = xs[0].shape[0]
    rows = own * parts

    def lanes(i, j):
        return pl.ds(pl.multiple_of(((z_self ^ j) * 4 + (p_self ^ i)) * block, block), block)

    gate = jnp.zeros((rows, span), F32)
    up = jnp.zeros((rows, span), F32)
    for i in range(4):
        x = jnp.concatenate(
            [jnp.concatenate([x_ref[:, lanes(i, j)] for x_ref in xs], axis=0) for j in range(4)],
            axis=1,
        )
        gate = gate + jnp.dot(x, gates[i][...], preferred_element_type=F32)
        up = up + jnp.dot(x, ups[i][...], preferred_element_type=F32)
    hidden = gate / (1.0 + jnp.exp(-gate)) * up
    keep = lax.broadcasted_iota(jnp.int32, (rows, span), 1) >= first_unit
    hidden = jnp.where(keep, hidden, 0.0).astype(BF)
    for i in range(4):
        down = jnp.concatenate([downs[i][j] for j in range(4)], axis=1)
        out = jnp.dot(hidden, down, preferred_element_type=F32).astype(BF)
        for j in range(4):
            for n, o_ref in enumerate(outs):
                o_ref[:, lanes(i, j)] = out[n * own : (n + 1) * own, j * block : (j + 1) * block]


def swap(x, axis, bit):
    size = lax.axis_size(axis)
    return lax.ppermute(x, axis, [(i, i ^ bit) for i in range(size)])


def plane_gather(x, first_bit):
    one, two = swap(x, "p", 1), swap(x, "p", 2)
    diag = swap(one, "p", 2) if first_bit == 1 else swap(two, "p", 1)
    return [x, one, two, diag]


def z_exchange(part):
    z_self = lax.axis_index("z")
    sends = [part(z_self ^ j) for j in range(1, 4)]
    got = [swap(x, "z", j + 1) for j, x in enumerate(sends)]
    return jnp.stack([part(z_self)] + got)


def fast_local(
    resid,
    queries,
    keys,
    values,
    lambdas,
    head_gain,
    out_weight,
    norm_gain,
    gate_weight,
    up_weight,
    down_weight,
):
    tok_rows, width = resid.shape
    own_rows = tok_rows // lax.axis_size("tp")
    z_self = lax.axis_index("z").astype(jnp.int32)
    p_self = lax.axis_index("p").astype(jnp.int32)

    def head(x):
        return lambda g: lax.dynamic_slice_in_dim(x, g * VD, VD, 1)

    qkv = z_exchange(lambda g: jnp.stack([head(x)(g) for x in (keys, values, queries)]))
    key_all = jnp.stack(plane_gather(qkv[:, 0], 1))
    value_all = jnp.stack(plane_gather(qkv[:, 1], 2))

    units = gate_weight.shape[1]
    span = -(-units // 512) * 128

    def start(g):
        return jnp.minimum(g * span, units - span)

    gate_mine = z_exchange(lambda g: lax.dynamic_slice_in_dim(gate_weight, start(g), span, 1))
    up_mine = z_exchange(lambda g: lax.dynamic_slice_in_dim(up_weight, start(g), span, 1))
    down_mine = z_exchange(lambda g: lax.dynamic_slice_in_dim(down_weight, start(g), span, 0))
    gates = plane_gather(gate_mine.reshape(-1, span), 1)
    ups = plane_gather(up_mine.reshape(-1, span), 2)
    half = span // 2
    low = plane_gather(down_mine[:, :half], 1)
    high = plane_gather(down_mine[:, half:], 2)
    downs = [jnp.concatenate(pair, axis=1) for pair in zip(low, high)]

    lam = lax.dynamic_slice_in_dim(lambdas, z_self, 1, 0)
    smem = pl.BlockSpec(memory_space=pltpu.SMEM)
    vmem = pl.BlockSpec(memory_space=pltpu.VMEM)
    keys_total = 16 * tok_rows
    attend = pl.pallas_call(
        functools.partial(attn_kernel, groups=4, planes=4, rows=tok_rows),
        out_shape=jax.ShapeDtypeStruct((4, tok_rows, VD), BF),
        in_specs=[smem, smem, vmem, vmem, vmem, vmem],
        out_specs=vmem,
        scratch_shapes=[pltpu.VMEM((2 * tok_rows, keys_total), F32)],
        cost_estimate=pl.CostEstimate(
            flops=3 * tok_rows * keys_total * 4 * VD * 2,
            transcendentals=5 * tok_rows * keys_total,
            bytes_accessed=4 * keys_total * VD,
        ),
        compiler_params=pltpu.CompilerParams(vmem_limit_bytes=40 * 1024 * 1024),
        name="attn",
    )
    place = jnp.stack([z_self, p_self])
    out = attend(place, lam, qkv[:, 2], key_all, value_all, head_gain.reshape(1, VD))
    back = z_exchange(lambda g: lax.dynamic_index_in_dim(out, g ^ z_self, 0, keepdims=False))
    head_out = jnp.concatenate(
        [lax.dynamic_index_in_dim(back, z_self ^ h, 0, keepdims=False) for h in range(4)], axis=1
    )
    projected = jnp.dot(head_out, out_weight, preferred_element_type=F32).astype(BF)
    t_self = lax.axis_index("tp")

    def half_rows(x, t):
        return lax.dynamic_slice_in_dim(x, t * own_rows, own_rows, 0)

    branch_in = swap(half_rows(projected, 1 - t_self), "tp", 1)
    branch = half_rows(projected, t_self).astype(F32) + branch_in.astype(F32)
    first = half_rows(resid, t_self).astype(F32) + branch
    scale = lax.rsqrt(jnp.mean(first * first, axis=-1, keepdims=True) + 1e-06)
    normed = (first * scale * norm_gain).astype(BF)
    mine = [normed] + [None] * 3
    for j in (3, 2, 1):
        mine[j] = swap(normed, "z", j)
    other = [swap(x, "tp", 1) for x in mine]
    first_unit = z_self * span - start(z_self)
    pos = jnp.stack([z_self, p_self, first_unit])

    def mix(slots):
        tokens = len(slots) * 2 * own_rows
        xs = [x for j in slots for x in (mine[j], other[j])]
        return pl.pallas_call(
            functools.partial(mixer_kernel, parts=len(xs)),
            out_shape=[jax.ShapeDtypeStruct((own_rows, width), BF)] * len(xs),
            in_specs=[smem] + [vmem] * (12 + len(xs)),
            out_specs=[vmem] * len(xs),
            cost_estimate=pl.CostEstimate(
                flops=6 * tokens * width * span,
                transcendentals=tokens * span,
                bytes_accessed=6 * width * span + 4 * tokens * width,
            ),
            compiler_params=pltpu.CompilerParams(vmem_limit_bytes=50 * 1024 * 1024),
            name="mixer",
        )(pos, *xs, *gates, *ups, *downs)

    def summed(keep, give):
        got = swap(give, "tp", 1)
        return keep.astype(F32) + got.astype(F32)

    far = mix((3, 2))
    sums = []
    for n, j in enumerate((3, 2)):
        part = summed(far[2 * n], far[2 * n + 1]).astype(BF)
        sums.append(swap(part, "z", j))
    near = mix((1, 0))
    part = summed(near[0], near[1]).astype(BF)
    sums.append(swap(part, "z", 1))
    mixer = summed(near[2], near[3])
    for part in sums:
        mixer = mixer + part.astype(F32)
    finished = (first + 0.5 * mixer).astype(BF)
    return lax.all_gather(finished, "tp", axis=0, tiled=True)


def attention_plain(queries, keys, values, lambdas, head_gain):
    tok_rows = queries.shape[0]
    local_heads = lambdas.shape[0]
    offset = (lax.axis_index("z") * lax.axis_size("p") + lax.axis_index("p")) * tok_rows
    query_four = queries.reshape(tok_rows, local_heads, 2, QK)
    query_pos = offset + lax.iota(jnp.int32, tok_rows)
    key_rows = lax.all_gather(keys, ("z", "p"), axis=0, tiled=True)
    value_rows = lax.all_gather(values, ("z", "p"), axis=0, tiled=True)
    key_count = key_rows.shape[0]
    key_span = key_count
    while key_span > 1024 and key_span % 2 == 0:
        key_span = key_span // 2

    def one_span(span_index, state):
        run_max, run_sum, run_acc = state
        start = span_index * key_span
        key_part = lax.dynamic_slice_in_dim(key_rows, start, key_span, 0)
        key_part = key_part.reshape(key_span, local_heads, 2, QK)
        value_part = lax.dynamic_slice_in_dim(value_rows, start, key_span, 0)
        value_part = value_part.reshape(key_span, local_heads, VD)
        key_pos = start + lax.iota(jnp.int32, key_span)
        scores = jnp.einsum("qhcd,khcd->chqk", query_four, key_part, preferred_element_type=F32)
        causal = key_pos[None, :] <= query_pos[:, None]
        scores = jnp.where(causal, scores * QK**-0.5, -1e30)
        new_max = jnp.maximum(run_max, jnp.max(scores, axis=-1))
        expo = jnp.where(causal, jnp.exp(scores - new_max[..., None]), 0.0)
        factor = jnp.exp(run_max - new_max)
        new_sum = run_sum * factor + jnp.sum(expo, axis=-1)
        new_acc = run_acc * factor[..., None] + jnp.einsum(
            "chqk,khd->chqd", expo.astype(BF), value_part, preferred_element_type=F32
        )
        return new_max, new_sum, new_acc

    initial = (
        jnp.full((2, local_heads, tok_rows), -1e30, F32),
        jnp.zeros((2, local_heads, tok_rows), F32),
        jnp.zeros((2, local_heads, tok_rows, VD), F32),
    )
    _, final_sum, final_acc = lax.fori_loop(0, key_count // key_span, one_span, initial)
    ratio = final_acc / final_sum[..., None]
    mixed = ratio[0] - lambdas[:, None, None] * ratio[1]
    scale = lax.rsqrt(jnp.mean(mixed * mixed, axis=-1, keepdims=True) + 1e-05)
    return (mixed * scale * head_gain).astype(BF)


def local(
    resid,
    queries,
    keys,
    values,
    lambdas,
    head_gain,
    out_weight,
    norm_gain,
    gate_weight,
    up_weight,
    down_weight,
):
    groups = lax.axis_size("z")
    planes = lax.axis_size("p")
    tok_rows, width = resid.shape
    local_heads = lambdas.shape[0]
    own_rows = tok_rows // lax.axis_size("tp")
    z_self = lax.axis_index("z")

    head_out = attention_plain(queries, keys, values, lambdas, head_gain)

    units = gate_weight.shape[1]
    span = -(-units // (groups * 128)) * 128
    starts = [min(g * span, units - span) for g in range(groups)]
    first_unit = z_self * span - jnp.minimum(z_self * span, units - span)
    k_rows = gate_weight.shape[0]

    gate_up = jnp.stack(
        [jnp.stack([gate_weight[:, s : s + span], up_weight[:, s : s + span]]) for s in starts]
    )
    gate_up = lax.all_to_all(gate_up, "z", 0, 0, tiled=True)
    gate_all = lax.all_gather(gate_up[:, 0], "p", axis=0, tiled=False).reshape(width, span)
    up_all = lax.all_gather(gate_up[:, 1], "p", axis=0, tiled=False).reshape(width, span)
    down = jnp.stack([down_weight[s : s + span] for s in starts])
    down = lax.all_to_all(down, "z", 0, 0, tiled=True)
    down_all = lax.all_gather(down, "p", axis=0, tiled=False)

    out_three = out_weight.reshape(local_heads, VD, width)
    branch = lax.psum_scatter(
        jnp.einsum("hqd,hde->qe", head_out, out_three, preferred_element_type=F32).astype(BF),
        "tp",
        scatter_dimension=0,
        tiled=True,
    ).astype(F32)
    resid_own = lax.dynamic_slice_in_dim(resid, lax.axis_index("tp") * own_rows, own_rows, 0)
    first = resid_own.astype(F32) + branch
    normed = first * lax.rsqrt(jnp.mean(first * first, axis=-1, keepdims=True) + 1e-06) * norm_gain
    normed = normed.astype(BF).reshape(own_rows, groups, planes, k_rows).transpose(0, 2, 1, 3)
    normed_all = lax.all_gather(normed.reshape(own_rows, width), ("z", "tp"), axis=0, tiled=True)
    gate_act = jnp.dot(normed_all, gate_all, preferred_element_type=F32)
    up_act = jnp.dot(normed_all, up_all, preferred_element_type=F32)
    keep = lax.iota(jnp.int32, span) >= first_unit
    hidden = jnp.where(keep[None, :], jax.nn.silu(gate_act) * up_act, 0.0).astype(BF)
    terms = jnp.einsum("th,pzhd->tzpd", hidden, down_all, preferred_element_type=F32)
    terms = terms.astype(BF).reshape(-1, width)
    mixer = lax.psum_scatter(terms, ("z", "tp"), scatter_dimension=0, tiled=True).astype(F32)
    finished = (first + 0.5 * mixer).astype(BF)
    return lax.all_gather(finished, "tp", axis=0, tiled=True)


def solution(mesh):
    sp, tp = mesh.shape["sp"], mesh.shape["tp"]
    groups = 4 if sp % 4 == 0 else 1
    split = Mesh(mesh.devices.reshape(groups, sp // groups, tp), ("z", "p", "tp"))
    rows = ("z", "p")

    def chosen(resid, queries, keys, values, lambdas, *rest):
        four = groups == 4 and sp // groups == 4 and lambdas.shape[0] == 4
        if four and rest[-1].shape[1] == 128:
            return fast_local(resid, queries, keys, values, lambdas, *rest)
        return local(resid, queries, keys, values, lambdas, *rest)

    return jax.shard_map(
        chosen,
        mesh=split,
        in_specs=(
            P(rows, None),
            P(rows, "tp"),
            P(rows, "tp"),
            P(rows, "tp"),
            P("tp"),
            P(),
            P("tp", None),
            P(),
            P(rows, "tp"),
            P(rows, "tp"),
            P("tp", rows),
        ),
        out_specs=P(rows, None),
        check_vma=False,
    )
```

```python
import functools

import jax
import jax.numpy as jnp
from jax import lax
from jax.experimental import pallas as pl
from jax.experimental.pallas import tpu as pltpu
from jax.sharding import Mesh, PartitionSpec as P


QK = 64
VD = 128
BF = jnp.bfloat16
F32 = jnp.float32


def attn_kernel(pos_ref, lam_ref, q_ref, k_ref, v_ref, gain_ref, o_ref, s_ref, *, groups, planes, rows):
    z_self = pos_ref[0]
    p_self = pos_ref[1]
    span = planes * rows
    lane = lax.broadcasted_iota(jnp.int32, (rows, 2 * QK), 1)
    row_id = lax.broadcasted_iota(jnp.int32, (rows, span), 0)
    col_id = lax.broadcasted_iota(jnp.int32, (rows, span), 1)
    mask_one = col_id <= row_id + p_self * rows
    mask = jnp.concatenate([mask_one, mask_one], axis=0)
    lam = lam_ref[0]
    for zq in range(groups):
        q = q_ref[z_self ^ zq] * jnp.asarray(QK**-0.5, BF)
        zero = jnp.zeros_like(q)
        q2 = jnp.concatenate([jnp.where(lane < QK, q, zero), jnp.where(lane < QK, zero, q)], axis=0)
        m = None
        for zk in range(zq + 1):
            kc = jnp.concatenate([k_ref[p_self ^ p, z_self ^ zk] for p in range(planes)], axis=0)
            s = lax.dot_general(q2, kc, (((1,), (1,)), ((), ())), preferred_element_type=F32)
            if zk == zq:
                s = jnp.where(mask, s, -1e30)
            s_ref[:, zk * span : (zk + 1) * span] = s
            mc = jnp.max(s, axis=-1, keepdims=True)
            m = mc if m is None else jnp.maximum(m, mc)
        acc = jnp.zeros((2 * rows, VD), F32)
        tot = jnp.zeros((2 * rows, 1), F32)
        for zk in range(zq + 1):
            e = jnp.exp(s_ref[:, zk * span : (zk + 1) * span] - m)
            tot = tot + jnp.sum(e, axis=-1, keepdims=True)
            vc = jnp.concatenate([v_ref[p_self ^ p, z_self ^ zk] for p in range(planes)], axis=0)
            acc = acc + jnp.dot(e.astype(BF), vc, preferred_element_type=F32)
        ratio = acc / tot
        mixed = ratio[:rows] - lam * ratio[rows:]
        scale = lax.rsqrt(jnp.mean(mixed * mixed, axis=-1, keepdims=True) + 1e-05)
        o_ref[z_self ^ zq] = (mixed * scale * gain_ref[...]).astype(BF)


def mixer_kernel(pos_ref, *refs, parts):
    xs, refs = refs[:parts], refs[parts:]
    pieces, outs = [refs[n : n + 4] for n in range(0, 28, 4)], refs[28:]
    gate_own, gate_rest, up_own, up_rest, down_own, down_low, down_high = pieces
    z_self, p_self, first_unit = pos_ref[0], pos_ref[1], pos_ref[2]
    block = down_own[0].shape[1]
    span = gate_own[0].shape[1]
    own = xs[0].shape[0]
    rows = own * parts

    def lanes(i, j):
        return pl.ds(pl.multiple_of(((z_self ^ j) * 4 + (p_self ^ i)) * block, block), block)

    gate = jnp.zeros((rows, span), F32)
    up = jnp.zeros((rows, span), F32)
    for i in range(4):
        x = jnp.concatenate(
            [jnp.concatenate([x_ref[:, lanes(i, j)] for x_ref in xs], axis=0) for j in range(4)],
            axis=1,
        )
        gate_w = jnp.concatenate([gate_own[i][...], gate_rest[i][...]], axis=0)
        up_w = jnp.concatenate([up_own[i][...], up_rest[i][...]], axis=0)
        gate = gate + jnp.dot(x, gate_w, preferred_element_type=F32)
        up = up + jnp.dot(x, up_w, preferred_element_type=F32)
    hidden = gate / (1.0 + jnp.exp(-gate)) * up
    keep = lax.broadcasted_iota(jnp.int32, (rows, span), 1) >= first_unit
    hidden = jnp.where(keep, hidden, 0.0).astype(BF)
    for i in range(4):
        rest = [jnp.concatenate([down_low[i][j], down_high[i][j]], axis=0) for j in range(3)]
        down = jnp.concatenate([down_own[i][...]] + rest, axis=1)
        out = jnp.dot(hidden, down, preferred_element_type=F32).astype(BF)
        for j in range(4):
            for n, o_ref in enumerate(outs):
                o_ref[:, lanes(i, j)] = out[n * own : (n + 1) * own, j * block : (j + 1) * block]


def swap(x, axis, bit):
    size = lax.axis_size(axis)
    return lax.ppermute(x, axis, [(i, i ^ bit) for i in range(size)])


def plane_gather(x, first_bit):
    one, two = swap(x, "p", 1), swap(x, "p", 2)
    diag = swap(one, "p", 2) if first_bit == 1 else swap(two, "p", 1)
    return [x, one, two, diag]


def z_exchange(part):
    z_self = lax.axis_index("z")
    sends = [part(z_self ^ j) for j in range(1, 4)]
    got = [swap(x, "z", j + 1) for j, x in enumerate(sends)]
    return part(z_self), got


def z_exchange_all(part):
    own, got = z_exchange(part)
    return jnp.stack([own] + got)


def fast_local(
    resid,
    queries,
    keys,
    values,
    lambdas,
    head_gain,
    out_weight,
    norm_gain,
    gate_weight,
    up_weight,
    down_weight,
):
    tok_rows, width = resid.shape
    own_rows = tok_rows // lax.axis_size("tp")
    z_self = lax.axis_index("z").astype(jnp.int32)
    p_self = lax.axis_index("p").astype(jnp.int32)

    def head(x):
        return lambda g: lax.dynamic_slice_in_dim(x, g * VD, VD, 1)

    qkv = z_exchange_all(lambda g: jnp.stack([head(x)(g) for x in (keys, values, queries)]))
    key_all = jnp.stack(plane_gather(qkv[:, 0], 1))
    value_all = jnp.stack(plane_gather(qkv[:, 1], 2))

    units = gate_weight.shape[1]
    span = -(-units // 512) * 128

    def start(g):
        return jnp.minimum(g * span, units - span)

    gate_own, gate_got = z_exchange(
        lambda g: lax.dynamic_slice_in_dim(gate_weight, start(g), span, 1)
    )
    up_own, up_got = z_exchange(lambda g: lax.dynamic_slice_in_dim(up_weight, start(g), span, 1))
    down_own, down_got = z_exchange(
        lambda g: lax.dynamic_slice_in_dim(down_weight, start(g), span, 0)
    )
    half = span // 2
    weights = (
        plane_gather(gate_own, 1)
        + plane_gather(jnp.concatenate(gate_got, axis=0), 1)
        + plane_gather(up_own, 2)
        + plane_gather(jnp.concatenate(up_got, axis=0), 2)
        + plane_gather(down_own, 1)
        + plane_gather(jnp.stack([x[:half] for x in down_got]), 1)
        + plane_gather(jnp.stack([x[half:] for x in down_got]), 2)
    )

    lam = lax.dynamic_slice_in_dim(lambdas, z_self, 1, 0)
    smem = pl.BlockSpec(memory_space=pltpu.SMEM)
    vmem = pl.BlockSpec(memory_space=pltpu.VMEM)
    keys_total = 16 * tok_rows
    attend = pl.pallas_call(
        functools.partial(attn_kernel, groups=4, planes=4, rows=tok_rows),
        out_shape=jax.ShapeDtypeStruct((4, tok_rows, VD), BF),
        in_specs=[smem, smem, vmem, vmem, vmem, vmem],
        out_specs=vmem,
        scratch_shapes=[pltpu.VMEM((2 * tok_rows, keys_total), F32)],
        cost_estimate=pl.CostEstimate(
            flops=3 * tok_rows * keys_total * 4 * VD * 2,
            transcendentals=5 * tok_rows * keys_total,
            bytes_accessed=4 * keys_total * VD,
        ),
        compiler_params=pltpu.CompilerParams(vmem_limit_bytes=40 * 1024 * 1024),
        name="attn",
    )
    place = jnp.stack([z_self, p_self])
    out = attend(place, lam, qkv[:, 2], key_all, value_all, head_gain.reshape(1, VD))
    back = z_exchange_all(lambda g: lax.dynamic_index_in_dim(out, g ^ z_self, 0, keepdims=False))
    head_out = jnp.concatenate(
        [lax.dynamic_index_in_dim(back, z_self ^ h, 0, keepdims=False) for h in range(4)], axis=1
    )
    projected = jnp.dot(head_out, out_weight, preferred_element_type=F32).astype(BF)
    t_self = lax.axis_index("tp")

    def half_rows(x, t):
        return lax.dynamic_slice_in_dim(x, t * own_rows, own_rows, 0)

    branch_in = swap(half_rows(projected, 1 - t_self), "tp", 1)
    branch = half_rows(projected, t_self).astype(F32) + branch_in.astype(F32)
    first = half_rows(resid, t_self).astype(F32) + branch
    scale = lax.rsqrt(jnp.mean(first * first, axis=-1, keepdims=True) + 1e-06)
    normed = (first * scale * norm_gain).astype(BF)
    mine = [normed] + [None] * 3
    mine[2] = swap(normed, "z", 2)
    mine[1] = swap(normed, "z", 1)
    mine[3] = swap(mine[2], "z", 1)
    other = [swap(x, "tp", 1) for x in mine]
    first_unit = z_self * span - start(z_self)
    pos = jnp.stack([z_self, p_self, first_unit])

    def mix(slots):
        tokens = len(slots) * 2 * own_rows
        xs = [x for j in slots for x in (mine[j], other[j])]
        return pl.pallas_call(
            functools.partial(mixer_kernel, parts=len(xs)),
            out_shape=[jax.ShapeDtypeStruct((own_rows, width), BF)] * len(xs),
            in_specs=[smem] + [vmem] * (len(weights) + len(xs)),
            out_specs=[vmem] * len(xs),
            cost_estimate=pl.CostEstimate(
                flops=6 * tokens * width * span,
                transcendentals=tokens * span,
                bytes_accessed=6 * width * span + 4 * tokens * width,
            ),
            compiler_params=pltpu.CompilerParams(vmem_limit_bytes=50 * 1024 * 1024),
            name="mixer",
        )(pos, *xs, *weights)

    def summed(keep, give):
        got = swap(give, "tp", 1)
        return keep.astype(F32) + got.astype(F32)

    keep, give = mix((3,))
    part = summed(keep, give).astype(BF)
    joined = swap(part, "z", 1)
    keep, give = mix((2,))
    part = (summed(keep, give) + joined.astype(F32)).astype(BF)
    from_two = swap(part, "z", 2)
    near = mix((1, 0))
    part = summed(near[0], near[1]).astype(BF)
    from_one = swap(part, "z", 1)
    mixer = summed(near[2], near[3]) + from_one.astype(F32) + from_two.astype(F32)
    finished = (first + 0.5 * mixer).astype(BF)
    return lax.all_gather(finished, "tp", axis=0, tiled=True)


def attention_plain(queries, keys, values, lambdas, head_gain):
    tok_rows = queries.shape[0]
    local_heads = lambdas.shape[0]
    offset = (lax.axis_index("z") * lax.axis_size("p") + lax.axis_index("p")) * tok_rows
    query_four = queries.reshape(tok_rows, local_heads, 2, QK)
    query_pos = offset + lax.iota(jnp.int32, tok_rows)
    key_rows = lax.all_gather(keys, ("z", "p"), axis=0, tiled=True)
    value_rows = lax.all_gather(values, ("z", "p"), axis=0, tiled=True)
    key_count = key_rows.shape[0]
    key_span = key_count
    while key_span > 1024 and key_span % 2 == 0:
        key_span = key_span // 2

    def one_span(span_index, state):
        run_max, run_sum, run_acc = state
        start = span_index * key_span
        key_part = lax.dynamic_slice_in_dim(key_rows, start, key_span, 0)
        key_part = key_part.reshape(key_span, local_heads, 2, QK)
        value_part = lax.dynamic_slice_in_dim(value_rows, start, key_span, 0)
        value_part = value_part.reshape(key_span, local_heads, VD)
        key_pos = start + lax.iota(jnp.int32, key_span)
        scores = jnp.einsum("qhcd,khcd->chqk", query_four, key_part, preferred_element_type=F32)
        causal = key_pos[None, :] <= query_pos[:, None]
        scores = jnp.where(causal, scores * QK**-0.5, -1e30)
        new_max = jnp.maximum(run_max, jnp.max(scores, axis=-1))
        expo = jnp.where(causal, jnp.exp(scores - new_max[..., None]), 0.0)
        factor = jnp.exp(run_max - new_max)
        new_sum = run_sum * factor + jnp.sum(expo, axis=-1)
        new_acc = run_acc * factor[..., None] + jnp.einsum(
            "chqk,khd->chqd", expo.astype(BF), value_part, preferred_element_type=F32
        )
        return new_max, new_sum, new_acc

    initial = (
        jnp.full((2, local_heads, tok_rows), -1e30, F32),
        jnp.zeros((2, local_heads, tok_rows), F32),
        jnp.zeros((2, local_heads, tok_rows, VD), F32),
    )
    _, final_sum, final_acc = lax.fori_loop(0, key_count // key_span, one_span, initial)
    ratio = final_acc / final_sum[..., None]
    mixed = ratio[0] - lambdas[:, None, None] * ratio[1]
    scale = lax.rsqrt(jnp.mean(mixed * mixed, axis=-1, keepdims=True) + 1e-05)
    return (mixed * scale * head_gain).astype(BF)


def local(
    resid,
    queries,
    keys,
    values,
    lambdas,
    head_gain,
    out_weight,
    norm_gain,
    gate_weight,
    up_weight,
    down_weight,
):
    groups = lax.axis_size("z")
    planes = lax.axis_size("p")
    tok_rows, width = resid.shape
    local_heads = lambdas.shape[0]
    own_rows = tok_rows // lax.axis_size("tp")
    z_self = lax.axis_index("z")

    head_out = attention_plain(queries, keys, values, lambdas, head_gain)

    units = gate_weight.shape[1]
    span = -(-units // (groups * 128)) * 128
    starts = [min(g * span, units - span) for g in range(groups)]
    first_unit = z_self * span - jnp.minimum(z_self * span, units - span)
    k_rows = gate_weight.shape[0]

    gate_up = jnp.stack(
        [jnp.stack([gate_weight[:, s : s + span], up_weight[:, s : s + span]]) for s in starts]
    )
    gate_up = lax.all_to_all(gate_up, "z", 0, 0, tiled=True)
    gate_all = lax.all_gather(gate_up[:, 0], "p", axis=0, tiled=False).reshape(width, span)
    up_all = lax.all_gather(gate_up[:, 1], "p", axis=0, tiled=False).reshape(width, span)
    down = jnp.stack([down_weight[s : s + span] for s in starts])
    down = lax.all_to_all(down, "z", 0, 0, tiled=True)
    down_all = lax.all_gather(down, "p", axis=0, tiled=False)

    out_three = out_weight.reshape(local_heads, VD, width)
    branch = lax.psum_scatter(
        jnp.einsum("hqd,hde->qe", head_out, out_three, preferred_element_type=F32).astype(BF),
        "tp",
        scatter_dimension=0,
        tiled=True,
    ).astype(F32)
    resid_own = lax.dynamic_slice_in_dim(resid, lax.axis_index("tp") * own_rows, own_rows, 0)
    first = resid_own.astype(F32) + branch
    normed = first * lax.rsqrt(jnp.mean(first * first, axis=-1, keepdims=True) + 1e-06) * norm_gain
    normed = normed.astype(BF).reshape(own_rows, groups, planes, k_rows).transpose(0, 2, 1, 3)
    normed_all = lax.all_gather(normed.reshape(own_rows, width), ("z", "tp"), axis=0, tiled=True)
    gate_act = jnp.dot(normed_all, gate_all, preferred_element_type=F32)
    up_act = jnp.dot(normed_all, up_all, preferred_element_type=F32)
    keep = lax.iota(jnp.int32, span) >= first_unit
    hidden = jnp.where(keep[None, :], jax.nn.silu(gate_act) * up_act, 0.0).astype(BF)
    terms = jnp.einsum("th,pzhd->tzpd", hidden, down_all, preferred_element_type=F32)
    terms = terms.astype(BF).reshape(-1, width)
    mixer = lax.psum_scatter(terms, ("z", "tp"), scatter_dimension=0, tiled=True).astype(F32)
    finished = (first + 0.5 * mixer).astype(BF)
    return lax.all_gather(finished, "tp", axis=0, tiled=True)


def solution(mesh):
    sp, tp = mesh.shape["sp"], mesh.shape["tp"]
    groups = 4 if sp % 4 == 0 else 1
    split = Mesh(mesh.devices.reshape(groups, sp // groups, tp), ("z", "p", "tp"))
    rows = ("z", "p")

    def chosen(resid, queries, keys, values, lambdas, *rest):
        four = groups == 4 and sp // groups == 4 and lambdas.shape[0] == 4
        if four and rest[-1].shape[1] == 128:
            return fast_local(resid, queries, keys, values, lambdas, *rest)
        return local(resid, queries, keys, values, lambdas, *rest)

    return jax.shard_map(
        chosen,
        mesh=split,
        in_specs=(
            P(rows, None),
            P(rows, "tp"),
            P(rows, "tp"),
            P(rows, "tp"),
            P("tp"),
            P(),
            P("tp", None),
            P(),
            P(rows, "tp"),
            P(rows, "tp"),
            P("tp", rows),
        ),
        out_specs=P(rows, None),
        check_vma=False,
    )
```
